32 devices in a mesh: sp: 8 (over z, x), tp: 4 (over y, core).
Axes of the slice: x: 2, y: 2, z: 4, core: 2. Of those that a mesh axis runs over, the one named last changes fastest.
Arguments:
- mid_state: bfloat16 [2048, 2048], P('sp'), may hold values from -6 to 6
- conv_pre: bfloat16 [2048, 1024], P('sp', 'tp'), may hold values from -8 to 8
- conv_taps: bfloat16 [31, 1024], P(None, 'tp'), may hold values from -1 to 1
- out_proj: bfloat16 [1024, 2048], P('tp'), may hold values from -0.1875 to 0.1875
- route_expert: int32 [2048, 2], P('sp'), may hold values from 0 to 7, as said below
- route_weight: float32 [2048, 2], P('sp'), may hold values from 0.1 to 1
- gate_w: bfloat16 [8, 2048, 2048], P('sp', None, 'tp'), may hold values from -0.125 to 0.125
- up_w: bfloat16 [8, 2048, 2048], P('sp', None, 'tp'), may hold values from -0.125 to 0.125
- down_w: bfloat16 [8, 2048, 2048], P('sp', 'tp'), may hold values from -0.125 to 0.125
- cotangent: bfloat16 [2048, 2048], P('sp'), may hold values from -6 to 6
Outputs:
- grad_gate: bfloat16 [8, 2048, 2048], P('sp', None, 'tp')
- grad_up: bfloat16 [8, 2048, 2048], P('sp', None, 'tp')
- grad_down: bfloat16 [8, 2048, 2048], P('sp', 'tp')
- grad_proj: float32 [2048, 1024], P('sp', 'tp')
- conv_input_grad: float32 [2048, 1024], P('sp', 'tp')
The draws below stay inside these ranges and needn't reach their ends.
Inputs may be any that keep to these rules, and one draw needn't show every extreme that they name: `route_expert`: the two experts of a token are different and lie in one group of 8 // 4 consecutive experts; in every draw some expert is named by more than 68 routes of every aligned block of 256 tokens.
All inputs are finite; a program needn't handle non-finite values.
Results may differ from the reference program's by a relative error of at most 0.02.
Values may be sent and summed in bfloat16 or wider, within the bound.
No kernel may reach another device: no remote copies, remote signals or barrier semaphores. Data moves between devices by JAX's collectives and lax.ppermute only.
A program may use at most 128 MiB of HBM per device.

```python
import jax
import jax.numpy as jnp
from jax import lax

D = 2048
FF = 2048
CONV = 1024
KERNEL = 31
TOP = 2
GROUPS = 4
TOK_DEV = 256
TOKENS = 2048
EXPERTS = 8
SLOTS = 68
N_TP = 4


def draw_route_expert(key, part):
    keys = jax.random.split(jax.random.fold_in(key, 17), 6)
    per_group = EXPERTS // GROUPS
    group_pick = jax.random.randint(keys[0], (TOKENS,), 0, GROUPS)
    first_pick = jax.random.randint(keys[1], (TOKENS,), 0, per_group)
    offset_pick = jax.random.randint(keys[2], (TOKENS,), 0, per_group - 1)
    second_pick = (first_pick + 1 + offset_pick) % per_group
    focus = jax.random.randint(keys[3], (), 0, EXPERTS)
    block_shift = jax.random.randint(keys[4], (TOKENS // TOK_DEV,), 0, TOK_DEV)
    row_ids = jnp.arange(TOKENS, dtype=jnp.int32)
    inside = (row_ids % TOK_DEV - block_shift[row_ids // TOK_DEV]) % TOK_DEV
    forced = inside <= SLOTS
    group_pick = jnp.where(forced, focus // per_group, group_pick)
    first_pick = jnp.where(forced, focus % per_group, first_pick)
    second_pick = jnp.where(forced, (focus % per_group + 1 + offset_pick) % per_group, second_pick)
    return jnp.stack([group_pick * per_group + first_pick, group_pick * per_group + second_pick], axis=1).astype(jnp.int32)


def with_spikes(result, own_key, source, target, blocks, factor):
    owner, partner = [(jnp.arange(result.shape[position]) // (result.shape[position] // blocks)).reshape([-1 if axis == position else 1 for axis in range(result.ndim)]) for position in (source, target)]
    chosen = jax.random.permutation(own_key, blocks)[partner]
    strong = (owner == chosen) | (owner == (partner + blocks // 2) % blocks)
    return jnp.where(strong, factor * result, result)


def levels(stream_key, shape, cuts, smallest, top_value):
    def one(axis_at, shards_of):
        steps = jax.random.uniform(jax.random.fold_in(jax.random.fold_in(stream_key, 6), axis_at), (shards_of,), jnp.float32, smallest / len(cuts), top_value / len(cuts))
        return jnp.repeat(jnp.exp(steps), shape[axis_at] // shards_of).reshape((-1,) + (1,) * (len(shape) - axis_at - 1))

    gain = one(*cuts[0])
    for cut in cuts[1:]:
        gain = gain * one(*cut)
    return gain


def bell_draw(rng, extent, scale, bound, pieces=(), kind=jnp.bfloat16):
    values = jax.random.normal(rng, extent, jnp.float32) * scale
    if len(pieces) > 0:
        values = levels(rng, extent, pieces, -0.22, 0.18) * values
    return jnp.clip(values, min=-bound, max=bound).astype(kind)


def heavy_noise(stream_key, shape, deviation, most, cuts, heavy, held_as=jnp.bfloat16):
    array = deviation * jax.random.normal(stream_key, shape, jnp.float32)
    if cuts:
        array = array * levels(stream_key, shape, cuts, -0.22, 0.18)
    return jnp.clip(with_spikes(array, jax.random.fold_in(stream_key, 3), *heavy), -most, most).astype(held_as)


def setup_inputs(seed: int = 0) -> dict:
    key_list = jax.random.split(jax.random.key(seed), 11)
    mid_state = bell_draw(key_list[0], (TOKENS, D), 1.0, 6.0, ((0, 8),))
    conv_pre = bell_draw(key_list[1], (TOKENS, CONV), 1.5, 8.0, ((0, 8), (1, 4)))
    conv_taps = bell_draw(key_list[2], (KERNEL, CONV), KERNEL ** -0.5, 1.0, ((1, 4),))
    out_proj = bell_draw(key_list[3], (CONV, D), CONV ** -0.5, 0.1875, ((0, 4),))
    route_expert = draw_route_expert(jax.random.fold_in(key_list[10], 71), 0)
    route_weight = jnp.clip(0.1 + 0.9 * jax.random.uniform(key_list[5], (TOKENS, TOP), jnp.float32) ** levels(key_list[5], (TOKENS, TOP), ((0, 8),), -0.2, 0.2), 0.1, 1.0)
    gate_w = bell_draw(key_list[6], (EXPERTS, D, FF), D ** -0.5, 0.125, ((0, 8), (2, 4)))
    up_w = bell_draw(key_list[7], (EXPERTS, D, FF), D ** -0.5, 0.125, ((0, 8), (2, 4)))
    down_w = bell_draw(key_list[8], (EXPERTS, FF, D), FF ** -0.5, 0.125, ((0, 8), (1, 4)))
    cotangent = heavy_noise(key_list[9], (TOKENS, D), 1.0, 6.0, ((0, 8),), (0, 1, 8, 2.0))
    return {"mid_state": mid_state, "conv_pre": conv_pre, "conv_taps": conv_taps, "out_proj": out_proj, "route_expert": route_expert, "route_weight": route_weight, "gate_w": gate_w, "up_w": up_w, "down_w": down_w, "cotangent": cotangent}


def silu_slope(value):
    sig = jax.nn.sigmoid(value)
    return sig * (1.0 + value * (1.0 - sig))


def expert_backward(packed):
    inputs, seeds, gate_mat, up_mat, down_mat = packed
    gate_pre = jnp.dot(inputs, gate_mat, preferred_element_type=jnp.float32)
    up_pre = jnp.dot(inputs, up_mat, preferred_element_type=jnp.float32)
    gate_act = jax.nn.silu(gate_pre)
    hidden = (gate_act * up_pre).astype(jnp.bfloat16)
    grad_down = jnp.dot(hidden.T, seeds, preferred_element_type=jnp.float32).astype(jnp.bfloat16)
    hidden_grad = jnp.dot(seeds, down_mat.T, preferred_element_type=jnp.float32)
    gate_grad = (hidden_grad * up_pre * silu_slope(gate_pre)).astype(jnp.bfloat16)
    up_grad = (hidden_grad * gate_act).astype(jnp.bfloat16)
    grad_gate = jnp.dot(inputs.T, gate_grad, preferred_element_type=jnp.float32).astype(jnp.bfloat16)
    grad_up = jnp.dot(inputs.T, up_grad, preferred_element_type=jnp.float32).astype(jnp.bfloat16)
    slot_total = inputs.shape[0]
    block_width = FF // N_TP
    gate_blocks = gate_grad.astype(jnp.float32).reshape(slot_total, N_TP, block_width)
    up_blocks = up_grad.astype(jnp.float32).reshape(slot_total, N_TP, block_width)
    gate_wblocks = gate_mat.astype(jnp.float32).reshape(D, N_TP, block_width)
    up_wblocks = up_mat.astype(jnp.float32).reshape(D, N_TP, block_width)
    partial_value = jnp.einsum("rjf,djf->rjd", gate_blocks, gate_wblocks) + jnp.einsum("rjf,djf->rjd", up_blocks, up_wblocks)
    partial_value = partial_value.astype(jnp.bfloat16).astype(jnp.float32)
    input_grad = jnp.sum(partial_value, axis=1).astype(jnp.bfloat16)
    return grad_gate, grad_up, grad_down, input_grad


def reference(mid_state, conv_pre, conv_taps, out_proj, route_expert, route_weight, gate_w, up_w, down_w, cotangent):
    blocks = TOKENS // TOK_DEV
    flat_routes = route_expert.reshape(-1)
    one_hot_table = (flat_routes[:, None] == jnp.arange(EXPERTS, dtype=jnp.int32)[None, :]).astype(jnp.int32)
    one_hot_table = one_hot_table.reshape(blocks, TOK_DEV * TOP, EXPERTS)
    slot_rank = (jnp.sum(jnp.cumsum(one_hot_table, axis=1) * one_hot_table, axis=2) - 1).reshape(-1)
    route_ids = jnp.arange(TOKENS * TOP, dtype=jnp.int32)
    source_block = route_ids // (TOK_DEV * TOP)
    token_ids = route_ids // TOP
    kept_mask = slot_rank < SLOTS
    per_expert = blocks * SLOTS
    slot_index = jnp.where(kept_mask, flat_routes * per_expert + source_block * SLOTS + slot_rank, EXPERTS * per_expert).astype(jnp.int32)
    route_cot = (route_weight.reshape(-1)[:, None] * cotangent[token_ids].astype(jnp.float32)).astype(jnp.bfloat16)
    slot_inputs = jnp.zeros((EXPERTS * per_expert, D), jnp.bfloat16).at[slot_index].set(mid_state[token_ids], mode="drop")
    slot_seeds = jnp.zeros((EXPERTS * per_expert, D), jnp.bfloat16).at[slot_index].set(route_cot, mode="drop")
    grad_gate, grad_up, grad_down, input_grad = lax.map(expert_backward, (slot_inputs.reshape(EXPERTS, per_expert, D), slot_seeds.reshape(EXPERTS, per_expert, D), gate_w, up_w, down_w))
    input_flat = input_grad.reshape(EXPERTS * per_expert, D)
    safe_index = jnp.minimum(slot_index, EXPERTS * per_expert - 1)
    returned = jnp.where(kept_mask[:, None], input_flat[safe_index].astype(jnp.float32), jnp.float32(0.0))
    moe_grad = jnp.sum(returned.reshape(TOKENS, TOP, D), axis=1)
    mid_grad = (cotangent.astype(jnp.float32) + moe_grad).astype(jnp.bfloat16)
    pre_float = conv_pre.astype(jnp.float32)
    activated = jax.nn.silu(pre_float).astype(jnp.bfloat16)
    grad_proj = jnp.dot(mid_grad.T, activated, preferred_element_type=jnp.float32)
    mixed_grad = jnp.dot(mid_grad, out_proj.T, preferred_element_type=jnp.float32)
    conv_grad = (mixed_grad * silu_slope(pre_float)).astype(jnp.bfloat16)
    extended = jnp.concatenate([conv_grad.astype(jnp.float32), jnp.zeros((KERNEL - 1, CONV), jnp.float32)], axis=0)
    conv_input_grad = jnp.zeros((TOKENS, CONV), jnp.float32)
    for lag_index in range(KERNEL):
        conv_input_grad = conv_input_grad + conv_taps[lag_index].astype(jnp.float32)[None, :] * extended[lag_index:lag_index + TOKENS]
    return grad_gate, grad_up, grad_down, grad_proj, conv_input_grad
```

```python
import functools

import jax
import jax.numpy as jnp
from jax import lax
from jax.experimental import pallas as pl
from jax.experimental.pallas import tpu as pltpu
from jax.sharding import PartitionSpec as P

D = 2048
KERNEL = 31
TOP = 2
GROUPS = 4
LANES = 128
BF = jnp.bfloat16
F32 = jnp.float32


def passed_along(value, axis, steps):
    count = lax.axis_size(axis)
    initial, last = (max(0, -steps), min(count, count - steps))
    return lax.ppermute(value, axis, [(source, source + steps) for source in range(initial, last)])


def silu_slope(value):
    sig = jax.nn.sigmoid(value)
    return sig * (1.0 + value * (1.0 - sig))


def mm(a, b):
    return lax.dot_general(a, b, (((1,), (0,)), ((), ())), preferred_element_type=F32)


def mm_nt(a, b):
    return lax.dot_general(a, b, (((1,), (1,)), ((), ())), preferred_element_type=F32)


def mm_tn(a, b):
    return lax.dot_general(a, b, (((0,), (0,)), ((), ())), preferred_element_type=F32)


def call(kernel, scalars, operands, outs, specs=None, flops=0, scratch=(), vmem=40 << 20, name=None):
    specs = specs or {}

    def whole(shape):
        zeros = (0,) * len(shape)
        return pl.BlockSpec(tuple(shape), lambda i, s, zeros=zeros: zeros)

    in_specs = [specs.get(n, whole(op.shape)) for n, op in enumerate(operands)]
    grid_spec = pltpu.PrefetchScalarGridSpec(
        num_scalar_prefetch=1,
        grid=(1,),
        in_specs=in_specs,
        out_specs=[whole(o.shape) for o in outs],
        scratch_shapes=list(scratch),
    )
    nbytes = sum(o.size * o.dtype.itemsize for o in outs) + sum(
        o.size * o.dtype.itemsize for o in operands
    )
    return pl.pallas_call(
        kernel,
        grid_spec=grid_spec,
        out_shape=list(outs),
        compiler_params=pltpu.CompilerParams(vmem_limit_bytes=vmem),
        cost_estimate=pl.CostEstimate(flops=int(flops), bytes_accessed=int(nbytes), transcendentals=0),
        name=name,
    )(scalars, *operands)


def sds(shape, dtype):
    return jax.ShapeDtypeStruct(tuple(shape), dtype)


def chunk_cols(tokens, quarters, which):
    return pl.BlockSpec((tokens, LANES), lambda i, s, which=which: (0, which * quarters + s[1]))


def dispatch_kernel(s, re, rw, *refs, slots, pad, nz):
    mids, cots = refs[:nz], refs[nz : 2 * nz]
    mid_out, cot_out, table = refs[2 * nz : 3 * nz], refs[3 * nz : 4 * nz], refs[4 * nz]
    tokens = re.shape[0]
    my_z = s[0]
    first = re[:, 0:1]
    rel = (first >> 1) - my_z
    rel = jnp.where(rel < 0, rel + nz, rel)
    lane = lax.broadcasted_iota(jnp.int32, (tokens, LANES), 1)
    member = jnp.where(rel == lane, 1.0, 0.0).astype(BF)
    er = lax.broadcasted_iota(jnp.int32, (LANES, LANES), 0)
    ec = lax.broadcasted_iota(jnp.int32, (LANES, LANES), 1)
    eye = jnp.where(er == ec, 1.0, 0.0).astype(BF)
    member_t = mm_nt(eye, member)
    ur = lax.broadcasted_iota(jnp.int32, (tokens, tokens), 0)
    uc = lax.broadcasted_iota(jnp.int32, (tokens, tokens), 1)
    upper = jnp.where(ur < uc, 1.0, 0.0).astype(BF)
    ranks = mm(member_t.astype(BF), upper)
    slot = lax.broadcasted_iota(jnp.int32, (LANES, tokens), 0).astype(F32)
    odd_first = (first & 1) == 1
    w0, w1 = rw[:, 0:1], rw[:, 1:2]
    parts = jnp.zeros((tokens, LANES), F32)
    for e, w in enumerate((jnp.where(odd_first, w1, w0), jnp.where(odd_first, w0, w1))):
        rest = w
        for n in range(3):
            piece = rest.astype(BF).astype(F32)
            rest = rest - piece
            parts = jnp.where(lane == 3 * e + n, piece, parts)
    parts = parts.astype(BF)
    pr = lax.broadcasted_iota(jnp.int32, (pad, LANES), 0)
    pc = lax.broadcasted_iota(jnp.int32, (pad, LANES), 1)
    rows_of = []
    for e in range(2):
        place = jnp.where((pr - slots == pc - 3 * e) & (pr >= slots) & (pr < slots + 3), 1.0, 0.0)
        rows_of.append(mm_nt(place.astype(BF), parts).astype(BF))
    mid = jnp.concatenate([m[...] for m in mids], axis=1)
    cot = jnp.concatenate([c[...] for c in cots], axis=1)
    for k in range(nz):
        hit = (member_t[k : k + 1, :] > 0.5) & (ranks[k : k + 1, :] == slot) & (slot < slots)
        full = jnp.where(hit, 1.0, 0.0)
        full_b = full.astype(BF)
        sel = full[:pad].astype(BF)
        table[k] = sel
        mid_out[k][...] = mm(sel, mid).astype(BF)
        rows = mm(sel, cot)
        extra = [mm_nt(rows_of[e], full_b) for e in range(2)]
        extra.append(jnp.zeros((pad, cot.shape[1] - 2 * LANES), F32))
        cot_out[k][...] = (rows + jnp.concatenate(extra, axis=1)).astype(BF)


def weight_rows(ref, index, nz, nt):
    return jnp.concatenate(
        [ref[pl.ds(pl.multiple_of((j * nt + index) * LANES, LANES), LANES), :] for j in range(nz)],
        axis=0,
    )


def weight_cols(ref, index, nz, nt):
    return jnp.concatenate(
        [ref[:, pl.ds(pl.multiple_of((j * nt + index) * LANES, LANES), LANES)] for j in range(nz)],
        axis=1,
    )


def forward_kernel(s, *refs, nz, nt):
    pieces, (gate, up), (gp, upre) = refs[:8], refs[8:10], refs[10:]
    half = pieces[0].shape[0]
    ins = [jnp.concatenate([pieces[4 * xx + r][...] for r in range(nt)], axis=1) for xx in range(2)]
    for w, out in ((gate, gp), (up, upre)):
        full = jnp.concatenate([weight_rows(w, s[1] ^ r, nz, nt) for r in range(nt)], axis=0)
        for xx in range(2):
            out[xx * half : (xx + 1) * half, :] = mm(ins[xx], full)


def hidden_kernel(s, *refs, nz, nt, slots, pad):
    pieces, (gp, upre, down) = refs[:8], refs[8:11]
    hidden, gg, ug, seeds = refs[11:]
    half = pieces[0].shape[0]
    odd = s[2] == 1
    row = lax.broadcasted_iota(jnp.int32, (pad, LANES), 0)
    col = lax.broadcasted_iota(jnp.int32, (pad, LANES), 1)
    full = [weight_cols(down, s[1] ^ r, nz, nt) for r in range(nt)]
    tail = lax.broadcasted_iota(jnp.int32, (pad, 2 * LANES), 0)
    for xx in range(2):
        cols = []
        for k in range(half // pad):
            block = pieces[4 * xx][k * pad : (k + 1) * pad, : 2 * LANES].astype(F32)
            line = jnp.sum(
                jnp.where((tail >= slots) & (tail < slots + 3), block, 0.0), axis=0, keepdims=True
            )
            line = jnp.where(odd, line[:, LANES:], line[:, :LANES])
            cols.append(jnp.sum(jnp.where(row == col, line, 0.0), axis=1, keepdims=True))
        weight = jnp.concatenate(cols, axis=0)
        acc = None
        for r in range(nt):
            seed = (pieces[4 * xx + r][...].astype(F32) * weight).astype(BF)
            seeds[r, xx * half : (xx + 1) * half, :] = seed
            part = mm_nt(seed, full[r])
            acc = part if acc is None else acc + part
        here = slice(xx * half, (xx + 1) * half)
        g = gp[here, :]
        u = upre[here, :]
        sig = jax.nn.sigmoid(g)
        act = g * sig
        hidden[here, :] = (act * u).astype(BF)
        gg[here, :] = (acc * u * (sig * (1.0 + g * (1.0 - sig)))).astype(BF)
        ug[here, :] = (acc * act).astype(BF)


def input_grad_of(s, gg, ug, gate, up, r, nz, nt):
    lhs = jnp.concatenate([gg[...], ug[...]], axis=1)
    rhs = jnp.concatenate(
        [weight_rows(gate, s[1] ^ r, nz, nt), weight_rows(up, s[1] ^ r, nz, nt)], axis=1
    )
    return mm_nt(lhs, rhs)


def partner_kernel(s, gg, ug, gate, up, out, *, nz, nt):
    for n, r in enumerate((1, 3)):
        out[n] = input_grad_of(s, gg, ug, gate, up, r, nz, nt).astype(BF)


def own_kernel(s, gg, ug, gate, up, got, q00, q10, q02, q12, *, nz, nt):
    half = q00.shape[0]
    for n, (r, outs) in enumerate(((0, (q00, q10)), (2, (q02, q12)))):
        total = input_grad_of(s, gg, ug, gate, up, r, nz, nt) + got[n].astype(F32)
        outs[0][...] = total[:half].astype(BF)
        outs[1][...] = total[half:].astype(BF)


def down_kernel(s, hidden, seeds, out, *, nz, nt):
    h = hidden[...]
    for r in range(nt):
        value = mm_tn(h, seeds[r]).astype(BF)
        for j in range(nz):
            at = pl.multiple_of((j * nt + (s[1] ^ r)) * LANES, LANES)
            out[:, pl.ds(at, LANES)] = value[:, j * LANES : (j + 1) * LANES]


def gate_up_kernel(s, *refs, nz, nt):
    pieces, (gg, ug), (out_g, out_u) = refs[:8], refs[8:10], refs[10:]
    for r in range(nt):
        rows = jnp.concatenate([pieces[r][...], pieces[4 + r][...]], axis=0)
        for grad, out in ((gg, out_g), (ug, out_u)):
            value = mm_tn(rows, grad[...]).astype(BF)
            for j in range(nz):
                at = pl.multiple_of((j * nt + (s[1] ^ r)) * LANES, LANES)
                out[pl.ds(at, LANES), :] = value[j * LANES : (j + 1) * LANES, :]


def settle_kernel(s, q, a, b, c, *outs, pad):
    for k, out in enumerate(outs):
        here = slice(k * pad, (k + 1) * pad)
        out[...] = (
            q[here, :].astype(F32) + a[here, :].astype(F32)
            + (b[here, :].astype(F32) + c[here, :].astype(F32))
        ).astype(BF)


def combine_kernel(s, *refs, nz):
    rets, table, cots = refs[:nz], refs[nz], refs[nz + 1 : 2 * nz + 1]
    mid_part, sends, keep = refs[2 * nz + 1], refs[2 * nz + 2 : 3 * nz + 2], refs[3 * nz + 2]
    moe = None
    for k in range(nz):
        part = mm_tn(table[k], rets[k][...])
        moe = part if moe is None else moe + part
    for j in range(nz):
        value = cots[j][...].astype(F32) + moe[:, j * LANES : (j + 1) * LANES]
        value = value.astype(BF)
        mid_part[:, j * LANES : (j + 1) * LANES] = value
        keep[j] = value
    for k in range(nz):
        j = s[0] + k
        j = jnp.where(j >= nz, j - nz, j)
        sends[k][...] = keep[j]


def conv_grad_kernel(s, m0, m1, m2, m3, proj, pre, out, *, nz, nt):
    lhs = jnp.concatenate([m0[...], m1[...], m2[...], m3[...]], axis=1)
    rhs = jnp.concatenate([weight_cols(proj, s[1] ^ r, nz, nt) for r in range(nt)], axis=1)
    out[...] = (mm_nt(lhs, rhs) * silu_slope(pre[...].astype(F32))).astype(BF)


def proj_kernel(s, a, b, ac, bc, act, out):
    at_a = (1 - (s[1] >> 1)) ^ s[2]
    at_b = (s[1] >> 1) ^ s[2]
    core = s[1] & 1
    act_a, act_b = act[at_a], act[at_b]
    for left, right, here in ((a, b, core), (ac, bc, 1 - core)):
        value = mm_tn(left[...], act_a) + mm_tn(right[...], act_b)
        out[pl.ds(pl.multiple_of(here * LANES, LANES), LANES), :] = value


def paired_body(
    mid_state,
    conv_pre,
    conv_taps,
    out_proj,
    route_expert,
    route_weight,
    gate_w,
    up_w,
    down_w,
    cotangent,
):
    groups, nt, nz = lax.axis_size("sp"), lax.axis_size("tp"), GROUPS
    tokens = mid_state.shape[0]
    slots = 17 * tokens * TOP // (16 * groups)
    pad = -(-(slots + 3) // 8) * 8
    width = D // nt
    half = nz * pad
    hid = gate_w.shape[2]
    sp, tp = lax.axis_index("sp"), lax.axis_index("tp")
    scal = jnp.stack([sp // TOP, tp, sp % TOP]).astype(jnp.int32)
    both = ("sp", "tp")

    def turn(value, k):
        perm = [(z * TOP + x, (z + k) % nz * TOP + x) for z in range(nz) for x in range(TOP)]
        return lax.ppermute(value, "sp", perm)

    def flip_x(value):
        return lax.ppermute(value, "sp", [(n, n ^ 1) for n in range(groups)])

    def flip_t(value, bit):
        return lax.ppermute(value, "tp", [(n, n ^ bit) for n in range(nt)])

    def joint(value, where):
        return lax.ppermute(
            value, both, [(n * nt + t, where(n, t)) for n in range(groups) for t in range(nt)]
        )

    def flip_d(value):
        return joint(value, lambda n, t: (n ^ 1) * nt + (t ^ 2))

    def spread(own):
        x1, y1, d1 = flip_x(own), flip_t(own, 2), flip_d(own)
        return [
            own, flip_t(own, 1), y1, flip_t(y1, 1), x1, flip_t(x1, 1), d1, flip_t(d1, 1),
        ]

    cols = [chunk_cols(tokens, nt, j) for j in range(nz)]
    specs = {2 + n: cols[n % nz] for n in range(2 * nz)}
    piece = sds((pad, width), BF)
    out = call(
        functools.partial(dispatch_kernel, slots=slots, pad=pad, nz=nz),
        scal,
        [route_expert, route_weight] + [mid_state] * nz + [cotangent] * nz,
        [piece] * (2 * nz) + [sds((nz, pad, tokens), BF)],
        specs,
        flops=4 * half * tokens * width,
        name="dispatch",
    )
    mid_send, cot_send, table = out[:nz], out[nz : 2 * nz], out[2 * nz]
    mid_got = [mid_send[0]] + [turn(mid_send[k], k) for k in range(1, nz)]
    cot_got = [cot_send[0]] + [turn(cot_send[k], k) for k in range(1, nz)]
    mid_in = spread(jnp.concatenate(mid_got, axis=0))
    cot_in = spread(jnp.concatenate(cot_got, axis=0))

    gate_mat, up_mat, down_mat = gate_w[0], up_w[0], down_w[0]
    rows = 2 * half
    wide = sds((rows, hid), F32)
    slim = sds((rows, hid), BF)
    gp, upre = call(
        functools.partial(forward_kernel, nz=nz, nt=nt),
        scal, mid_in + [gate_mat, up_mat], [wide, wide], flops=4 * rows * D * hid, name="forward",
    )
    gp, conv_late = lax.optimization_barrier((gp, conv_pre))
    hidden, gg, ug, seeds = call(
        functools.partial(hidden_kernel, nz=nz, nt=nt, slots=slots, pad=pad),
        scal, cot_in + [gp, upre, down_mat],
        [slim, slim, slim, sds((nt, rows, width), BF)], flops=2 * rows * D * hid, name="hidden",
    )
    (to_partner,) = call(
        functools.partial(partner_kernel, nz=nz, nt=nt),
        scal, [gg, ug, gate_mat, up_mat], [sds((2, rows, width), BF)],
        flops=2 * rows * D * hid, name="partner",
    )
    from_partner = flip_t(to_partner, 1)
    (grad_down,) = call(
        functools.partial(down_kernel, nz=nz, nt=nt),
        scal, [hidden, seeds], [sds((hid, D), BF)], flops=2 * rows * D * hid, name="down",
    )
    part = sds((half, width), BF)
    q00, q10, q02, q12 = call(
        functools.partial(own_kernel, nz=nz, nt=nt),
        scal, [gg, ug, gate_mat, up_mat, from_partner], [part] * 4,
        flops=2 * rows * D * hid, name="own",
    )
    rx, ry, rd = flip_x(q10), flip_t(q02, 2), flip_d(q12)
    grad_gate, grad_up = call(
        functools.partial(gate_up_kernel, nz=nz, nt=nt),
        scal, mid_in + [gg, ug], [sds((D, hid), BF)] * 2, flops=4 * rows * D * hid, name="gateup",
    )
    settled = call(
        functools.partial(settle_kernel, pad=pad), scal, [q00, rx, ry, rd], [piece] * nz, name="settle",
    )
    rets = [settled[0]] + [turn(settled[k], nz - k) for k in range(1, nz)]
    specs = {nz + 1 + n: cols[n] for n in range(nz)}
    out = call(
        functools.partial(combine_kernel, nz=nz),
        scal, rets + [table] + [cotangent] * nz,
        [sds((tokens, width), BF)] + [sds((tokens, LANES), BF)] * nz,
        specs, flops=2 * half * tokens * width,
        scratch=[pltpu.VMEM((nz, tokens, LANES), BF)], name="combine",
    )
    mid_part, sends = out[0], out[1:]

    m1, m2 = flip_t(mid_part, 1), flip_t(mid_part, 2)
    m3 = flip_t(m2, 1)
    (conv_grad,) = call(
        functools.partial(conv_grad_kernel, nz=nz, nt=nt),
        scal, [mid_part, m1, m2, m3, out_proj, conv_pre], [sds(conv_pre.shape, BF)],
        flops=2 * tokens * D * conv_pre.shape[1], name="convgrad",
    )
    next_head = passed_along(conv_grad[: KERNEL - 1], "sp", -1)
    extended = jnp.concatenate([conv_grad, next_head], axis=0).astype(F32)
    conv_input_grad = jnp.zeros(conv_grad.shape, F32)
    for lag_index in range(KERNEL):
        conv_input_grad = (
            conv_input_grad
            + conv_taps[lag_index].astype(F32)[None, :]
            * extended[lag_index : lag_index + tokens]
        )

    pre2 = jnp.concatenate([conv_late, flip_x(conv_late)], axis=0)
    pres = [pre2] + [turn(pre2, k) for k in range(1, nz)]
    act = jnp.stack(
        [jnp.concatenate([p[x * tokens : (x + 1) * tokens] for p in pres], axis=0) for x in range(2)]
    )
    act = jax.nn.silu(act.astype(F32)).astype(BF)
    have = jnp.concatenate([sends[0]] + [turn(sends[k], k) for k in range(1, nz)], axis=0)

    def near(n, t):
        x, y, c = n % TOP, t >> 1, t & 1
        return (n - x + y) * nt + (1 - x) * 2 + c

    def far(n, t):
        x, y, c = n % TOP, t >> 1, t & 1
        return (n - x + y) * nt + x * 2 + c

    got_a, got_b = joint(have, near), joint(have, far)
    (grad_proj,) = call(
        proj_kernel,
        scal, [got_a, got_b, flip_t(got_a, 1), flip_t(got_b, 1), act],
        [sds((2 * LANES, conv_pre.shape[1]), F32)],
        flops=2 * tokens * groups * 2 * LANES * conv_pre.shape[1], name="proj",
    )
    return (grad_gate[None], grad_up[None], grad_down[None], grad_proj, conv_input_grad)


def body(
    mid_state,
    conv_pre,
    conv_taps,
    out_proj,
    route_expert,
    route_weight,
    gate_w,
    up_w,
    down_w,
    cotangent,
):
    groups = lax.axis_size("sp")
    token_count = mid_state.shape[0]
    slot_count = 17 * token_count * TOP // (16 * groups)
    flat_routes = route_expert.reshape(-1)
    one_hot_table = (flat_routes[:, None] == jnp.arange(groups, dtype=jnp.int32)[None, :]).astype(
        jnp.int32
    )
    slot_rank = jnp.sum(jnp.cumsum(one_hot_table, axis=0) * one_hot_table, axis=1) - 1
    kept_mask = slot_rank < slot_count
    slot_index = jnp.where(kept_mask, flat_routes * slot_count + slot_rank, groups * slot_count)
    token_ids = jnp.arange(token_count * TOP, dtype=jnp.int32) // TOP
    route_cot = (
        route_weight.reshape(-1)[:, None] * cotangent[token_ids].astype(jnp.float32)
    ).astype(jnp.bfloat16)
    send_inputs = (
        jnp.zeros((groups * slot_count, D), jnp.bfloat16)
        .at[slot_index]
        .set(mid_state[token_ids], mode="drop")
        .reshape(groups, slot_count, D)
    )
    send_seeds = (
        jnp.zeros((groups * slot_count, D), jnp.bfloat16)
        .at[slot_index]
        .set(route_cot, mode="drop")
        .reshape(groups, slot_count, D)
    )
    got_inputs, got_seeds = (
        lax.all_to_all(send_inputs, "sp", split_axis=0, concat_axis=0, tiled=True),
        lax.all_to_all(send_seeds, "sp", split_axis=0, concat_axis=0, tiled=True),
    )
    inputs = got_inputs.reshape(groups * slot_count, D)
    seeds = got_seeds.reshape(groups * slot_count, D)
    gate_mat = gate_w[0]
    up_mat = up_w[0]
    down_mat = down_w[0]
    gate_pre = jnp.dot(inputs, gate_mat, preferred_element_type=jnp.float32)
    up_pre = jnp.dot(inputs, up_mat, preferred_element_type=jnp.float32)
    gate_act = jax.nn.silu(gate_pre)
    hidden = (gate_act * up_pre).astype(jnp.bfloat16)
    hidden_grad = lax.dot_general(
        seeds, down_mat, (((1,), (1,)), ((), ())), preferred_element_type=jnp.float32
    )
    gate_grad = (hidden_grad * up_pre * silu_slope(gate_pre)).astype(jnp.bfloat16)
    up_grad = (hidden_grad * gate_act).astype(jnp.bfloat16)
    grad_down = lax.dot_general(
        hidden, seeds, (((0,), (0,)), ((), ())), preferred_element_type=jnp.float32
    ).astype(jnp.bfloat16)
    grad_gate = lax.dot_general(
        inputs, gate_grad, (((0,), (0,)), ((), ())), preferred_element_type=jnp.float32
    ).astype(jnp.bfloat16)
    grad_up = lax.dot_general(
        inputs, up_grad, (((0,), (0,)), ((), ())), preferred_element_type=jnp.float32
    ).astype(jnp.bfloat16)
    weight_results = (grad_gate, grad_up, grad_down)
    partial_value = lax.dot_general(
        gate_grad, gate_mat, (((1,), (1,)), ((), ())), preferred_element_type=jnp.float32
    )
    partial_value = partial_value + lax.dot_general(
        up_grad, up_mat, (((1,), (1,)), ((), ())), preferred_element_type=jnp.float32
    )
    partial_value = partial_value.astype(jnp.bfloat16).astype(jnp.float32)
    safe_index = jnp.minimum(slot_index, groups * slot_count - 1)
    slice_width = D // lax.axis_size("tp")
    summed = lax.psum_scatter(
        partial_value.astype(jnp.bfloat16), "tp", scatter_dimension=1, tiled=True
    )
    returned = lax.all_to_all(
        summed.reshape(groups, slot_count, slice_width),
        "sp",
        split_axis=0,
        concat_axis=0,
        tiled=True,
    ).reshape(groups * slot_count, slice_width)
    picked = jnp.where(
        kept_mask[:, None], returned[safe_index].astype(jnp.float32), jnp.float32(0.0)
    )
    moe_grad = jnp.sum(picked.reshape(token_count, TOP, slice_width), axis=1)
    own_cot = lax.dynamic_slice_in_dim(
        cotangent, lax.axis_index("tp") * slice_width, slice_width, 1
    )
    mid_part = (own_cot.astype(jnp.float32) + moe_grad).astype(jnp.bfloat16)
    mid_grad = lax.all_gather(mid_part, "tp", axis=1, tiled=True)
    grad_gate, grad_up, grad_down = weight_results
    pre_float = conv_pre.astype(jnp.float32)
    activated = jax.nn.silu(pre_float).astype(jnp.bfloat16)
    mixed_grad = lax.dot_general(
        mid_grad, out_proj, (((1,), (1,)), ((), ())), preferred_element_type=jnp.float32
    )
    conv_grad = (mixed_grad * silu_slope(pre_float)).astype(jnp.bfloat16)
    next_head = passed_along(conv_grad[: KERNEL - 1], "sp", -1)
    extended = jnp.concatenate([conv_grad, next_head], axis=0).astype(jnp.float32)
    conv_input_grad = jnp.zeros(conv_grad.shape, jnp.float32)
    for lag_index in range(KERNEL):
        conv_input_grad = (
            conv_input_grad
            + conv_taps[lag_index].astype(jnp.float32)[None, :]
            * extended[lag_index : lag_index + token_count]
        )
    grad_proj = lax.psum_scatter(
        lax.dot_general(
            mid_grad, activated, (((0,), (0,)), ((), ())), preferred_element_type=jnp.float32
        ).astype(jnp.bfloat16),
        "sp",
        scatter_dimension=0,
        tiled=True,
    ).astype(jnp.float32)
    return (grad_gate[None], grad_up[None], grad_down[None], grad_proj, conv_input_grad)


def solution(mesh):
    placed = (
        P("sp", None),
        P("sp", "tp"),
        P(None, "tp"),
        P("tp", None),
        P("sp", None),
        P("sp", None),
        P("sp", None, "tp"),
        P("sp", None, "tp"),
        P("sp", "tp", None),
        P("sp", None),
    )
    paired = (
        mesh.shape["sp"] == GROUPS * TOP
        and mesh.shape["tp"] == 4
        and D == GROUPS * mesh.shape["tp"] * LANES
    )
    return jax.shard_map(
        paired_body if paired else body,
        mesh=mesh,
        in_specs=placed,
        out_specs=(
            P("sp", None, "tp"),
            P("sp", None, "tp"),
            P("sp", "tp", None),
            P("sp", "tp"),
            P("sp", "tp"),
        ),
        check_vma=False,
    )
```
